512 devices in a mesh: sp: 64 (over z, y), tp: 8 (over x, core).
Axes of the slice: x: 4, y: 4, z: 16, core: 2. Of those that a mesh axis runs over, the one named last changes fastest.
Arguments:
- tokens: bfloat16 [65536, 2048], P('sp', 'tp'), may hold values from -6 to 6
- norm_gain: float32 [2048], replicated, may hold values from 0.1 to 1.9
- w_query: bfloat16 [2048, 1024], P('sp', 'tp'), may hold values from -0.125 to 0.125
- w_key: bfloat16 [2048, 512], P('sp', 'tp'), may hold values from -0.125 to 0.125
- w_value: bfloat16 [2048, 512], P('sp', 'tp'), may hold values from -0.125 to 0.125
- w_glu_a: bfloat16 [2048, 1024], P('sp', 'tp'), may hold values from -0.125 to 0.125
- w_glu_b: bfloat16 [2048, 1024], P('sp', 'tp'), may hold values from -0.125 to 0.125
- q_gain: float32 [64], replicated, may hold values from 0.8 to 7
- k_gain: float32 [64], replicated, may hold values from 0.8 to 7
- sink_logit: float32 [16], P('tp'), may hold values from 1 to 4
- conv_taps: float32 [31, 1024], P(None, 'tp'), may hold values from -1 to 1
- chan_gain: float32 [1024], P('tp'), may hold values from 0.1 to 1.9
- chan_bias: float32 [1024], P('tp'), may hold values from -3 to 3
- w_attn_back: bfloat16 [2048, 1024], P('sp', 'tp'), may hold values from -0.1875 to 0.1875
- w_conv_back: bfloat16 [2048, 1024], P('sp', 'tp'), may hold values from -0.1875 to 0.1875
Outputs:
- mixed: bfloat16 [65536, 2048], P(('sp', 'tp'))
- log_weight: float32 [16, 65536], P('tp', 'sp')
The draws below stay inside these ranges and needn't reach their ends.
All inputs are finite; a program needn't handle non-finite values.
Results may differ from the reference program's by a relative error of at most 0.014.
The reference program's roundings to bfloat16 on the way count: a program that leaves them out, or rounds other values in their place, can miss the bound.
Values may be sent and summed in bfloat16 or wider, within the bound.
A program may use at most 128 MiB of HBM per device.

```python
import jax
import jax.numpy as jnp
from jax import lax

D = 2048
HEAD = 64
Q_HEADS = 16
KV_HEADS = 8
CH = 1024
KW = 31
WINDOW = 128
TOKENS = 65536
N_TP = 8


def draw_q_gain(key, part):
    own_key = jax.random.fold_in(key, 11)
    return jax.random.uniform(own_key, (HEAD,), jnp.float32, 0.8, 1.2)


def draw_k_gain(key, part):
    own_key = jax.random.fold_in(key, 23)
    return jax.random.uniform(own_key, (HEAD,), jnp.float32, 0.8, 1.2)


def levels(rng, dims, split, least, high):
    gain = 1.0
    for dim, parts in split:
        draws = jax.random.uniform(jax.random.fold_in(jax.random.fold_in(rng, 6), dim), (parts,), jnp.float32, least / len(split), high / len(split))
        gain = gain * jnp.repeat(jnp.exp(draws), dims[dim] // parts).reshape((-1,) + (1,) * (len(dims) - 1 - dim))
    return gain


def normal_values(rng, extent, deviation, most, shards=(), held_as=jnp.bfloat16):
    drawn = deviation * jax.random.normal(rng, extent, jnp.float32)
    if shards:
        drawn = drawn * levels(rng, extent, shards, -0.22, 0.18)
    return jnp.clip(drawn, -most, most).astype(held_as)


def setup_inputs(seed: int = 0) -> dict:
    streams_of = jax.random.split(jax.random.key(seed), 16)
    return {
        "tokens": normal_values(streams_of[0], (TOKENS, D), 1.0, 6.0, ((0, 64), (1, 8))),
        "norm_gain": jnp.clip(1.0 + 0.18 * jax.random.normal(streams_of[1], (D,), jnp.float32), 0.1, 1.9),
        "w_query": normal_values(streams_of[2], (D, Q_HEADS * HEAD), D ** -0.5, 0.125, ((0, 64), (1, 8))),
        "w_key": normal_values(streams_of[3], (D, KV_HEADS * HEAD), D ** -0.5, 0.125, ((0, 64), (1, 8))),
        "w_value": normal_values(streams_of[4], (D, KV_HEADS * HEAD), D ** -0.5, 0.125, ((0, 64), (1, 8))),
        "w_glu_a": normal_values(streams_of[5], (D, CH), D ** -0.5, 0.125, ((0, 64), (1, 8))),
        "w_glu_b": normal_values(streams_of[6], (D, CH), D ** -0.5, 0.125, ((0, 64), (1, 8))),
        "q_gain": draw_q_gain(jax.random.fold_in(streams_of[15], 71), 0),
        "k_gain": draw_k_gain(jax.random.fold_in(streams_of[15], 71), 0),
        "sink_logit": jnp.clip(1.0 + 3.0 * jax.random.uniform(streams_of[9], (Q_HEADS,), jnp.float32) ** levels(streams_of[9], (Q_HEADS,), ((0, 8),), -0.2, 0.2), 1.0, 4.0),
        "conv_taps": normal_values(streams_of[10], (KW, CH), KW ** -0.5, 1.0, ((1, 8),), jnp.float32),
        "chan_gain": jnp.clip(1.0 + 0.18 * jax.random.normal(streams_of[11], (CH,), jnp.float32), 0.1, 1.9),
        "chan_bias": normal_values(streams_of[12], (CH,), 0.5, 3.0, ((0, 8),), jnp.float32),
        "w_attn_back": normal_values(streams_of[13], (D, Q_HEADS * HEAD), (Q_HEADS * HEAD) ** -0.5, 0.1875, ((0, 64), (1, 8))),
        "w_conv_back": normal_values(streams_of[14], (D, CH), CH ** -0.5, 0.1875, ((0, 64), (1, 8))),
    }


EPS = 1e-06

def row_norm(inputs, scale_vec):
    squares = lax.optimization_barrier(jnp.mean(inputs * inputs, axis=-1, keepdims=True))
    return inputs * lax.rsqrt(squares + EPS) * scale_vec

def reference(tokens, norm_gain, w_query, w_key, w_value, w_glu_a, w_glu_b, q_gain, k_gain, sink_logit, conv_taps, chan_gain, chan_bias, w_attn_back, w_conv_back):
    seq_total = tokens.shape[0]
    group_size = Q_HEADS // KV_HEADS
    normed = row_norm(tokens.astype(jnp.float32), norm_gain).astype(jnp.bfloat16)
    query_raw = jnp.dot(normed, w_query, preferred_element_type=jnp.float32)
    key_raw = jnp.dot(normed, w_key, preferred_element_type=jnp.float32)
    value_raw = jnp.dot(normed, w_value, preferred_element_type=jnp.float32)
    glu_a = jnp.dot(normed, w_glu_a, preferred_element_type=jnp.float32)
    glu_b = jnp.dot(normed, w_glu_b, preferred_element_type=jnp.float32)
    queries = row_norm(query_raw.reshape(seq_total, Q_HEADS, HEAD), q_gain).astype(jnp.bfloat16)
    key_rows = row_norm(key_raw.reshape(seq_total, KV_HEADS, HEAD), k_gain).astype(jnp.bfloat16)
    value_rows = value_raw.astype(jnp.bfloat16).reshape(seq_total, KV_HEADS, HEAD)
    gated_rows = (glu_a * jax.nn.sigmoid(glu_b)).astype(jnp.bfloat16)
    zero_keys = jnp.zeros((WINDOW, KV_HEADS, HEAD), jnp.bfloat16)
    keys_padded = jnp.concatenate([zero_keys, key_rows], 0)
    values_padded = jnp.concatenate([zero_keys, value_rows], 0)
    offsets = jnp.arange(WINDOW, dtype=jnp.int32)
    band_offsets = jnp.arange(2 * WINDOW, dtype=jnp.int32)
    distance = WINDOW + offsets[:, None] - band_offsets[None, :]
    allowed = (distance >= 0) & (distance < WINDOW)
    sink_table = sink_logit.reshape(KV_HEADS, group_size)[:, :, None, None]

    def one_block(block_index):
        block_start = (block_index * WINDOW).astype(jnp.int32)
        query_block = lax.dynamic_slice_in_dim(queries, block_start, WINDOW, 0).astype(jnp.float32)
        query_block = query_block.reshape(WINDOW, KV_HEADS, group_size, HEAD)
        key_band = lax.dynamic_slice_in_dim(keys_padded, block_start, 2 * WINDOW, 0).astype(jnp.float32)
        value_band = lax.dynamic_slice_in_dim(values_padded, block_start, 2 * WINDOW, 0).astype(jnp.float32)
        scores = jnp.einsum('qhgd,khd->hgqk', query_block, key_band) * HEAD ** (-0.5)
        visible = allowed & (block_start - WINDOW + band_offsets[None, :] >= 0)
        masked = jnp.where(visible, scores, -jnp.inf)
        largest = jnp.maximum(lax.optimization_barrier(jnp.max(masked, axis=-1, keepdims=True)), sink_table)
        weights = jnp.where(visible, jnp.exp(scores - largest), 0.0)
        weight_sum = lax.optimization_barrier(jnp.sum(weights, axis=-1, keepdims=True)) + jnp.exp(sink_table - largest)
        log_sum = (largest + jnp.log(weight_sum))[..., 0].reshape(Q_HEADS, WINDOW)
        probabilities = (weights / weight_sum).astype(jnp.bfloat16)
        mixed_rows = jnp.einsum('hgqk,khd->qhgd', probabilities.astype(jnp.float32), value_band)
        return (mixed_rows.astype(jnp.bfloat16).reshape(WINDOW, Q_HEADS * HEAD), log_sum)
    block_count = seq_total // WINDOW
    attended, log_sums = lax.map(one_block, jnp.arange(block_count, dtype=jnp.int32))
    attended = attended.reshape(seq_total, Q_HEADS * HEAD)
    log_weight = jnp.transpose(log_sums, (1, 0, 2)).reshape(Q_HEADS, seq_total)
    zero_rim = jnp.zeros((KW - 1, CH), jnp.float32)
    extended = jnp.concatenate([zero_rim, gated_rows.astype(jnp.float32)], 0)
    convolved = jnp.zeros((seq_total, CH), jnp.float32)
    for tap_index in range(KW):
        convolved = convolved + conv_taps[tap_index] * extended[tap_index:tap_index + seq_total]
    center = lax.optimization_barrier(jnp.mean(convolved, axis=-1, keepdims=True))
    spread = lax.optimization_barrier(jnp.mean(convolved * convolved, axis=-1, keepdims=True)) - center * center
    normal = (convolved - center) * lax.rsqrt(spread + EPS) * chan_gain + chan_bias
    conv_rows = jax.nn.silu(normal).astype(jnp.bfloat16)
    attn_cols = Q_HEADS * HEAD // N_TP
    conv_cols = CH // N_TP
    summed = jnp.zeros((seq_total, D), jnp.float32)
    for shard_index in range(N_TP):
        attn_lo = shard_index * attn_cols
        conv_lo = shard_index * conv_cols
        partial_sum = jnp.dot(attended[:, attn_lo:attn_lo + attn_cols], w_attn_back[:, attn_lo:attn_lo + attn_cols].T, preferred_element_type=jnp.float32)
        partial_sum = partial_sum + jnp.dot(conv_rows[:, conv_lo:conv_lo + conv_cols], w_conv_back[:, conv_lo:conv_lo + conv_cols].T, preferred_element_type=jnp.float32)
        rounded = lax.optimization_barrier(partial_sum.astype(jnp.bfloat16))
        summed = summed + rounded.astype(jnp.float32)
    return (summed.astype(jnp.bfloat16), log_weight)
```

```python
import functools

import jax
import jax.numpy as jnp
from jax import lax
from jax.experimental import pallas as pl
from jax.experimental.pallas import tpu as pltpu
from jax.sharding import PartitionSpec as P

MESH = pl.DeviceIdType.MESH
HEAD = 64
CH = 1024
KW = 31
WINDOW = 128
EPS = 1e-06
NX, NC, NY = 4, 2, 4
LANES = 128
RIM = 32
PIECES = 4
BF = jnp.bfloat16
F32 = jnp.float32


def kernel(
    nz,
    tok_in,
    norm_gain,
    w_query,
    w_key,
    w_value,
    w_glu_a,
    w_glu_b,
    q_gain,
    k_gain,
    sink,
    conv_taps,
    chan_gain,
    chan_bias,
    w_attn_back,
    w_conv_back,
    out,
    log_weight,
    tok,
    nrm,
    wa,
    wb,
    qp,
    kvx,
    ext,
    conv,
    act,
    stats,
    lines,
    own,
    snd,
    pre,
    relay_a,
    relay_b,
    fin,
    tok_sem,
    own_d2d,
    x_sem,
    xr_sem,
    d2d_sem,
    ya_sem,
    up_a,
    dn_a,
    up_b,
    dn_b,
    by_r,
    by_l,
    br_r,
    br_l,
    halo_sem,
    stat_sem,
    pre_sem,
    rs_sem,
):
    sp = lax.axis_index("sp")
    tp = lax.axis_index("tp")
    n_sp = nz * NY
    z, y = sp // NY, sp % NY
    x, c = tp // NC, tp % NC
    rows = tok_in.shape[0]
    half = nz // 2
    piece = rows // PIECES
    pending = []

    def at(zz, yy, xx, cc):
        return (lax.rem(zz + nz, nz) * NY + lax.rem(yy + NY, NY), lax.rem(xx + NX, NX) * NC + cc)

    def send(src, dst, sems, index, where):
        copy = pltpu.make_async_remote_copy(
            src_ref=src,
            dst_ref=dst,
            send_sem=sems.at[(0, *index)],
            recv_sem=sems.at[(1, *index)],
            device_id=where,
            device_id_type=MESH,
        )
        copy.start()
        pending.append(copy)

    def landed(ref, sems, index):
        pltpu.make_async_remote_copy(
            src_ref=ref,
            dst_ref=ref,
            send_sem=sems.at[(0, *index)],
            recv_sem=sems.at[(1, *index)],
            device_id=partner,
            device_id_type=MESH,
        ).wait_recv()

    z_up, z_dn = at(z + 1, y, x, c), at(z - 1, y, x, c)
    y_up, y_dn = at(z, y + 1, x, c), at(z, y - 1, x, c)
    x_up, x_dn = at(z, y, x + 1, c), at(z, y, x - 1, c)
    partner = (sp, x * NC + (1 - c))
    following = (lax.rem(sp + 1, n_sp), tp)
    preceding = (lax.rem(sp + n_sp - 1, n_sp), tp)

    load = pltpu.make_async_copy(tok_in, tok.at[tp], tok_sem)
    load.start()

    def weight_rows(zz, yy):
        block = lax.rem(zz + 2 * nz, nz) * NY + lax.rem(yy + NY, NY)
        return pl.ds(pl.multiple_of(block * 32, 32), 32)

    mine = weight_rows(z, y)
    wa[mine, :LANES] = w_query[...]
    wa[mine, LANES:] = jnp.concatenate([w_key[...], w_value[...]], axis=1)
    wb[mine, :LANES] = w_glu_a[...]
    wb[mine, LANES : 2 * LANES] = w_glu_b[...]
    wb[mine, 2 * LANES : 3 * LANES] = w_attn_back[...]
    wb[mine, 3 * LANES :] = w_conv_back[...]

    barrier = pltpu.get_barrier_semaphore()
    peers = [(sp, lax.rem(tp + k, NX * NC)) for k in range(1, NX * NC)]
    peers += [at(z, y + k, x, c) for k in range(1, NY)]
    peers += [z_up, z_dn, following, preceding]
    for peer in peers:
        pl.semaphore_signal(barrier, inc=1, device_id=peer, device_id_type=MESH)
    pl.semaphore_wait(barrier, len(peers))

    def wa_at(zz, yy):
        return wa.at[weight_rows(zz, yy)]

    def wb_at(zz, yy):
        return wb.at[weight_rows(zz, yy)]

    offsets = (0, 1, 3, 2)

    def a_up(step, j):
        if step < half - 1 or (step == half - 1 and j < 2):
            block = wa_at(z - step, y - offsets[j])
            send(block, block, up_a, (step, j), z_up)

    def a_dn(step, j):
        if step < half - 1 or (step == half - 1 and j >= 2):
            block = wa_at(z + step, y - offsets[j])
            send(block, block, dn_a, (step, j), z_dn)

    def b_up(step):
        if step < half:
            block = wb_at(z - step, y)
            send(block, block, up_b, (step,), z_up)

    def b_dn(step):
        if step < half - 1:
            block = wb_at(z + step, y)
            send(block, block, dn_b, (step,), z_dn)

    def shift(n):
        return -n - 1 if n < half else n - half

    def b_y(n):
        block = wb_at(z + shift(n), y)
        send(block, block, by_r, (n,), y_up)
        send(block, block, by_l, (n,), y_dn)

    def b_relay(n):
        if n < half:
            block = wb_at(z + shift(n), y - 1)
            landed(block, by_r, (n,))
            send(block, block, br_r, (n,), y_up)
        else:
            block = wb_at(z + shift(n), y + 1)
            landed(block, by_l, (n,))
            send(block, block, br_l, (n - half,), y_dn)

    a_up(0, 0)
    a_dn(0, 0)
    for k in (1, 3, 2):
        send(wa_at(z, y), wa_at(z, y), ya_sem, (k,), at(z, y + k, x, c))
    b_up(0)
    b_dn(0)
    b_y(half)

    def tok_at(xx, cc, i):
        return tok.at[lax.rem(xx + NX, NX) * NC + cc, pl.ds(i * piece, piece)]

    load.wait()
    order_up, order_dn = (0, 1, 2, 3), (2, 3, 0, 1)
    for i, j in zip(order_up, order_dn):
        send(tok_at(x, c, i), tok_at(x, c, i), x_sem, (0, i), x_up)
        send(tok_at(x, c, j), tok_at(x, c, j), x_sem, (1, j), x_dn)
    send(tok.at[tp], tok.at[tp], own_d2d, (), partner)

    def to_partner(k, xx, i):
        send(tok_at(xx, c, i), tok_at(xx, c, i), d2d_sem, (k, i), partner)

    def tokens_step(n):
        if n < PIECES:
            i, j = order_up[n], order_dn[n]
            landed(tok_at(x - 1, c, i), x_sem, (0, i))
            if n < PIECES // 2:
                send(tok_at(x - 1, c, i), tok_at(x - 1, c, i), xr_sem, (i,), x_up)
            to_partner(0, x - 1, i)
            landed(tok_at(x + 1, c, j), x_sem, (1, j))
            if n < PIECES // 2:
                send(tok_at(x + 1, c, j), tok_at(x + 1, c, j), xr_sem, (j,), x_dn)
            to_partner(1, x + 1, j)
        elif n < PIECES + PIECES // 2:
            for i in (order_up[n - PIECES], order_dn[n - PIECES]):
                landed(tok_at(x + 2, c, i), xr_sem, (i,))
                to_partner(2, x + 2, i)

    for j in range(1, NY):
        k = offsets[j]
        landed(wa_at(z, y - k), ya_sem, (k,))
        a_up(0, j)
        a_dn(0, j)
    for step in range(half):
        landed(wb_at(z - step - 1, y), up_b, (step,))
        b_up(step + 1)
        b_y(step)
        if step < half - 1:
            landed(wb_at(z + step + 1, y), dn_b, (step,))
            b_dn(step + 1)
            b_y(half + step + 1)
        for j in range(NY):
            if step < half - 1 or j < 2:
                landed(wa_at(z - step - 1, y - offsets[j]), up_a, (step, j))
                a_up(step + 1, j)
            if step < half - 1 or j >= 2:
                landed(wa_at(z + step + 1, y - offsets[j]), dn_a, (step, j))
                a_dn(step + 1, j)
        b_relay(half + step)
        if step > 0:
            b_relay(step - 1)
        if step > 0:
            tokens_step(step - 1)
    b_relay(half - 1)
    for n in range(half - 1, PIECES + PIECES // 2):
        tokens_step(n)

    landed(tok.at[x * NC + 1 - c], own_d2d, ())
    for k, xx in ((0, x - 1), (1, x + 1), (2, x + 2)):
        for i in range(PIECES):
            landed(tok_at(xx, 1 - c, i), d2d_sem, (k, i))

    tile = 128
    gains = [norm_gain[i : i + 1, :] for i in range(NX * NC)]

    def norm_tile(t, carry):
        at_rows = pl.ds(pl.multiple_of(t * tile, tile), tile)
        total = jnp.zeros((tile, 256), F32)
        for i in range(NX * NC):
            v = tok[i, at_rows, :].astype(F32)
            total = total + v * v
        scale = lax.rsqrt(jnp.sum(total, axis=1, keepdims=True) * (1.0 / 2048) + EPS)
        for i in range(NX * NC):
            v = tok[i, at_rows, :].astype(F32)
            nrm[at_rows, i * 256 : (i + 1) * 256] = (v * scale * gains[i]).astype(BF)
        return carry

    lax.fori_loop(0, rows // tile, norm_tile, 0)

    for n in range(half, 2 * half):
        landed(wb_at(z + shift(n), y - 1), by_r, (n,))
    for n in range(half):
        landed(wb_at(z + shift(n), y + 1), by_l, (n,))
    for n in range(half):
        landed(wb_at(z + shift(n), y + 2), br_r, (n,))
        landed(wb_at(z + shift(half + n), y + 2), br_l, (n,))

    big = 256
    low = lax.broadcasted_iota(jnp.int32, (big, LANES), 1) < HEAD

    def project(t):
        at_rows = pl.ds(pl.multiple_of(t * big, big), big)
        normed = nrm[at_rows, :]
        first = jnp.dot(normed, wa[...], preferred_element_type=F32)
        second = jnp.dot(normed, wb[:, :256], preferred_element_type=F32)
        q, kv = first[:, :LANES], first[:, LANES:]
        squares = q * q
        mean0 = jnp.sum(jnp.where(low, squares, 0.0), axis=1, keepdims=True) * (1.0 / HEAD)
        mean1 = jnp.sum(jnp.where(low, 0.0, squares), axis=1, keepdims=True) * (1.0 / HEAD)
        qn = q * jnp.where(low, lax.rsqrt(mean0 + EPS), lax.rsqrt(mean1 + EPS)) * q_gain[...]
        qp[0, at_rows, :] = jnp.where(low, qn, 0.0).astype(BF)
        qp[1, at_rows, :] = jnp.where(low, pltpu.roll(qn, HEAD, 1), 0.0).astype(BF)
        mean = jnp.sum(jnp.where(low, kv * kv, 0.0), axis=1, keepdims=True) * (1.0 / HEAD)
        kn = kv * lax.rsqrt(mean + EPS) * k_gain[...]
        kvx[pl.ds(pl.multiple_of(t * big + WINDOW, WINDOW), big), :] = jnp.where(low, kn, kv).astype(BF)
        a, b = second[:, :LANES], second[:, LANES:]
        gated = (a * (1.0 / (1.0 + jnp.exp(-b)))).astype(BF).astype(F32)
        ext[pl.ds(pl.multiple_of(t * big + RIM, RIM), big), :] = gated

    tiles = rows // big
    project(tiles - 1)
    send(kvx.at[pl.ds(rows, WINDOW)], kvx.at[pl.ds(0, WINDOW)], halo_sem, (0,), following)
    send(ext.at[pl.ds(rows, RIM)], ext.at[pl.ds(0, RIM)], halo_sem, (1,), following)

    def project_step(t, carry):
        project(t)
        return carry

    lax.fori_loop(0, tiles - 1, project_step, 0)
    landed(ext.at[pl.ds(0, RIM)], halo_sem, (1,))
    ext[:RIM, :] = jnp.where(sp > 0, ext[:RIM, :], 0.0)

    eye = lax.broadcasted_iota(jnp.int32, (LANES, LANES), 0) == lax.broadcasted_iota(
        jnp.int32, (LANES, LANES), 1
    )
    blocks = rows // LANES
    for t in range(blocks):
        total = jnp.zeros((LANES, LANES), F32)
        for j in range(KW):
            start = t * LANES + RIM - (KW - 1) + j
            total = total + conv_taps[j : j + 1, :] * ext[start : start + LANES, :]
        conv[t * LANES : (t + 1) * LANES, :] = total
        for k, terms in enumerate((total, total * total)):
            column = jnp.sum(terms, axis=1, keepdims=True)
            line = jnp.sum(jnp.where(eye, column, 0.0), axis=0, keepdims=True)
            stats[tp, k * blocks + t : k * blocks + t + 1, :] = line
    for k in range(1, NX * NC):
        send(stats.at[tp], stats.at[tp], stat_sem, (k,), (sp, lax.rem(tp + k, NX * NC)))
    landed(kvx.at[pl.ds(0, WINDOW)], halo_sem, (0,))

    hq = 2 * WINDOW
    key_index = lax.broadcasted_iota(jnp.int32, (hq, hq), 0)
    query_index = lax.rem(lax.broadcasted_iota(jnp.int32, (hq, hq), 1), WINDOW)
    band = (key_index > query_index) & (key_index <= query_index + WINDOW)
    lane_row = lax.broadcasted_iota(jnp.int32, (1, hq), 1)
    sinks = jnp.where(lane_row < WINDOW, sink[0], sink[1])
    low_w = lax.broadcasted_iota(jnp.int32, (WINDOW, LANES), 1) < HEAD

    def attend(b):
        r0 = pl.multiple_of(b * WINDOW, WINDOW)
        keys = kvx[pl.ds(r0, hq), :]
        queries = jnp.concatenate([qp[0, pl.ds(r0, WINDOW), :], qp[1, pl.ds(r0, WINDOW), :]], axis=0)
        scores = lax.dot_general(keys, queries, (((1,), (1,)), ((), ())), preferred_element_type=F32)
        scores = scores * HEAD ** (-0.5)
        least = jnp.where(sp * rows + b * WINDOW > 0, 0, WINDOW)
        visible = band & (key_index >= least)
        largest = jnp.max(jnp.where(visible, scores, -jnp.inf), axis=0, keepdims=True)
        largest = jnp.maximum(largest, sinks)
        weights = jnp.where(visible, jnp.exp(scores - largest), 0.0)
        weight_sum = jnp.sum(weights, axis=0, keepdims=True) + jnp.exp(sinks - largest)
        line = largest + jnp.log(weight_sum)
        log_weight[0:1, pl.ds(r0, WINDOW)] = line[:, :WINDOW]
        log_weight[1:2, pl.ds(r0, WINDOW)] = line[:, WINDOW:]
        shares = (weights * (1.0 / weight_sum)).astype(BF)
        mixed = lax.dot_general(shares, keys, (((0,), (0,)), ((), ())), preferred_element_type=F32)
        mixed = jnp.where(low_w, pltpu.roll(mixed[:WINDOW], HEAD, 1), mixed[WINDOW:])
        act[pl.ds(r0, WINDOW), :LANES] = mixed.astype(BF)

    def channel_norm(t, center, scale):
        at_rows = pl.ds(pl.multiple_of(t * LANES, LANES), LANES)
        columns = []
        for lines in (center, scale):
            columns.append(jnp.sum(jnp.where(eye, lines, 0.0), axis=1, keepdims=True))
        normal = (conv[at_rows, :] - columns[0]) * columns[1] * chan_gain[...] + chan_bias[...]
        act[at_rows, LANES:] = (normal * (1.0 / (1.0 + jnp.exp(-normal)))).astype(BF)

    def attend_group(o):
        g = lax.rem(x + o, NX)

        def one(i, carry):
            attend(g * NC + i)
            return carry

        lax.fori_loop(0, NC, one, 0)

    def project_back(o):
        g = lax.rem(x + o, NX)
        for i in range(NC):
            t = g * NC + i
            channel_norm(t, lines[pl.ds(t, 1), :], lines[pl.ds(t + blocks, 1), :])
        keep = act[pl.ds(pl.multiple_of((g * NC + c) * LANES, LANES), LANES), :]
        give = act[pl.ds(pl.multiple_of((g * NC + 1 - c) * LANES, LANES), LANES), :]
        both = jnp.concatenate([keep, give], axis=0)
        for n in range(4):
            cols = slice(n * 512, (n + 1) * 512)
            part = lax.dot_general(
                both, wb[cols, 256:], (((1,), (1,)), ((), ())), preferred_element_type=F32
            ).astype(BF)
            own[o, :, cols] = part[:LANES]
            snd[o, :, cols] = part[LANES:]
        send(snd.at[o], pre.at[o], pre_sem, (o,), partner)

    attend_group(2)
    for k in range(1, NX * NC):
        other = lax.rem(tp + NX * NC - k, NX * NC)
        landed(stats.at[other], stat_sem, (k,))
    sums = jnp.sum(stats[...], axis=0)
    center = sums[:blocks] * (1.0 / CH)
    spread = sums[blocks:] * (1.0 / CH) - center * center
    lines[:blocks, :] = center
    lines[blocks:, :] = lax.rsqrt(spread + EPS)

    project_back(2)
    hr = LANES // 2

    def pair(o, lo):
        return own[o, lo : lo + hr, :].astype(F32) + pre[o, lo : lo + hr, :].astype(F32)

    attend_group(1)
    project_back(1)
    landed(pre.at[2], pre_sem, (2,))
    own[2, :hr, :] = pair(2, 0).astype(BF)
    send(own.at[2, pl.ds(0, hr)], relay_a, rs_sem, (0,), x_up)
    own[2, hr:, :] = pair(2, hr).astype(BF)
    send(own.at[2, pl.ds(hr, hr)], relay_b, rs_sem, (1,), x_dn)
    attend_group(3)
    project_back(3)
    landed(pre.at[1], pre_sem, (1,))
    own[1, hr:, :] = pair(1, hr).astype(BF)
    send(own.at[1, pl.ds(hr, hr)], fin.at[0, pl.ds(hr, hr)], rs_sem, (2,), x_up)
    landed(pre.at[3], pre_sem, (3,))
    own[3, :hr, :] = pair(3, 0).astype(BF)
    send(own.at[3, pl.ds(0, hr)], fin.at[1, pl.ds(0, hr)], rs_sem, (3,), x_dn)
    attend_group(0)
    project_back(0)
    landed(relay_a, rs_sem, (0,))
    own[1, :hr, :] = (pair(1, 0) + relay_a[...].astype(F32)).astype(BF)
    send(own.at[1, pl.ds(0, hr)], fin.at[0, pl.ds(0, hr)], rs_sem, (4,), x_up)
    landed(relay_b, rs_sem, (1,))
    own[3, hr:, :] = (pair(3, hr) + relay_b[...].astype(F32)).astype(BF)
    send(own.at[3, pl.ds(hr, hr)], fin.at[1, pl.ds(hr, hr)], rs_sem, (5,), x_dn)
    landed(pre.at[0], pre_sem, (0,))
    for lo, first, second in ((hr, (0, 2), (1, 5)), (0, (1, 3), (0, 4))):
        for k, i in (first, second):
            landed(fin.at[k, pl.ds(lo, hr)], rs_sem, (i,))
        total = pair(0, lo)
        for k in range(2):
            total = total + fin[k, lo : lo + hr, :].astype(F32)
        out[lo : lo + hr, :] = total.astype(BF)

    for copy in pending:
        copy.wait_send()


def local(
    tokens,
    norm_gain,
    w_query,
    w_key,
    w_value,
    w_glu_a,
    w_glu_b,
    q_gain,
    k_gain,
    sink_logit,
    conv_taps,
    chan_gain,
    chan_bias,
    w_attn_back,
    w_conv_back,
):
    rows, width = tokens.shape
    model = norm_gain.shape[0]
    nz = lax.axis_size("sp") // NY
    half = nz // 2
    n_tp = NX * NC
    blocks = rows // LANES
    vmem = pl.BlockSpec(memory_space=pltpu.VMEM)
    dma = pltpu.SemaphoreType.DMA
    return pl.pallas_call(
        functools.partial(kernel, nz),
        out_shape=(
            jax.ShapeDtypeStruct((LANES, model), BF),
            jax.ShapeDtypeStruct((2, rows), F32),
        ),
        in_specs=[pl.BlockSpec(memory_space=pltpu.HBM)]
        + [vmem] * 8
        + [pl.BlockSpec(memory_space=pltpu.SMEM)]
        + [vmem] * 5,
        out_specs=(vmem, vmem),
        scratch_shapes=[
            pltpu.VMEM((n_tp, rows, width), BF),
            pltpu.VMEM((rows, model), BF),
            pltpu.VMEM((model, 256), BF),
            pltpu.VMEM((model, 512), BF),
            pltpu.VMEM((2, rows, LANES), BF),
            pltpu.VMEM((rows + WINDOW, LANES), BF),
            pltpu.VMEM((rows + RIM, LANES), F32),
            pltpu.VMEM((rows, LANES), F32),
            pltpu.VMEM((rows, 256), BF),
            pltpu.VMEM((n_tp, 2 * blocks, LANES), F32),
            pltpu.VMEM((2 * blocks, LANES), F32),
            pltpu.VMEM((NX, LANES, model), BF),
            pltpu.VMEM((NX, LANES, model), BF),
            pltpu.VMEM((NX, LANES, model), BF),
            pltpu.VMEM((LANES // 2, model), BF),
            pltpu.VMEM((LANES // 2, model), BF),
            pltpu.VMEM((2, LANES, model), BF),
            dma,
            dma((2,)),
            dma((2, 2, PIECES)),
            dma((2, PIECES)),
            dma((2, 3, PIECES)),
            dma((2, NY)),
            dma((2, half, NY)),
            dma((2, half, NY)),
            dma((2, half)),
            dma((2, half)),
            dma((2, 2 * half)),
            dma((2, 2 * half)),
            dma((2, half)),
            dma((2, half)),
            dma((2, 2)),
            dma((2, n_tp)),
            dma((2, NX)),
            dma((2, 6)),
        ],
        compiler_params=pltpu.CompilerParams(
            collective_id=0, has_side_effects=True, vmem_limit_bytes=60 * 1024 * 1024
        ),
    )(
        tokens,
        norm_gain.reshape(n_tp, width),
        w_query,
        w_key,
        w_value,
        w_glu_a,
        w_glu_b,
        jnp.concatenate([q_gain, q_gain]).reshape(1, LANES),
        jnp.concatenate([k_gain, k_gain]).reshape(1, LANES),
        sink_logit,
        conv_taps,
        chan_gain.reshape(1, LANES),
        chan_bias.reshape(1, LANES),
        w_attn_back,
        w_conv_back,
    )


def solution(mesh):
    return jax.shard_map(
        local,
        mesh=mesh,
        in_specs=(
            P("sp", "tp"),
            P(),
            P("sp", "tp"),
            P("sp", "tp"),
            P("sp", "tp"),
            P("sp", "tp"),
            P("sp", "tp"),
            P(),
            P(),
            P("tp"),
            P(None, "tp"),
            P("tp"),
            P("tp"),
            P("sp", "tp"),
            P("sp", "tp"),
        ),
        out_specs=(P(("sp", "tp"), None), P("tp", "sp")),
        check_vma=False,
    )
```
